32 devices in a mesh: sp: 8 (over z, y), tp: 4 (over x, core).
Axes of the slice: x: 2, y: 2, z: 4, core: 2. Of those that a mesh axis runs over, the one named last changes fastest.
Arguments:
- query_input: bfloat16 [4096, 1024], P('sp', 'tp'), may hold values from -6 to 6
- value_input: bfloat16 [4096, 1024], P('sp', 'tp'), may hold values from -6 to 6
- forget_ahead: bfloat16 [4096, 1024], P('sp', 'tp'), may hold values from -7.5 to 7.5
- forget_behind: bfloat16 [4096, 1024], P('sp', 'tp'), may hold values from -7.5 to 7.5
- output_gate: bfloat16 [4096, 1024], P('sp', 'tp'), may hold values from -6 to 6
- floor_ahead: float32 [1024], P('tp'), may hold values from 0.9 to 0.99996094
- floor_behind: float32 [1024], P('tp'), may hold values from 0.9 to 0.99996094
- head_gain: float32 [1024], P('tp'), may hold values from 0.1 to 1.9
- decay_jolts: float32 [8, 4096], P('tp', 'sp'), may hold values from -2.1 to 0
- residual: bfloat16 [4096, 2048], P(('sp', 'tp')), may hold values from -6 to 6
- out_weight: bfloat16 [1024, 2048], replicated, may hold values from -0.1875 to 0.1875
- norm_gain: float32 [2048], replicated, may hold values from 0.1 to 1.9
- norm_bias: float32 [2048], replicated, may hold values from -1.5 to 1.5
- expert_ids: int32 [4096, 2], P('sp'), may hold values from 0 to 7, all different within a row; in each aligned block of 128 rows (0 to 127, 128 to 255, ...) at most 64 rows name the same one
- route_scale: float32 [4096, 2], P('sp'), may hold values from 0.3 to 1.5
- expert_gate: bfloat16 [8, 2048, 512], P('sp', None, 'tp'), may hold values from -0.125 to 0.125
- expert_up: bfloat16 [8, 2048, 512], P('sp', None, 'tp'), may hold values from -0.125 to 0.125
- expert_down: bfloat16 [8, 512, 2048], P('sp', 'tp'), may hold values from -0.25 to 0.25
- shared_gate: bfloat16 [2048, 512], P(None, 'tp'), may hold values from -0.125 to 0.125
- shared_up: bfloat16 [2048, 512], P(None, 'tp'), may hold values from -0.125 to 0.125
- shared_down: bfloat16 [512, 2048], P('tp'), may hold values from -0.25 to 0.25
Outputs:
- layer_output: bfloat16 [4096, 2048], P(('sp', 'tp'))
The draws below stay inside these ranges and needn't reach their ends.
Inputs may be any that keep to these rules, and one draw needn't show every extreme that they name: `expert_ids`: A position's 2 experts differ. In each aligned block of 128 positions no expert is named by more than 64 of the block's positions, and in some block one expert is named by exactly 64; every expert is named somewhere.
All inputs are finite; a program needn't handle non-finite values.
Results may differ from the reference program's by a relative error of at most 0.015.
Values may be sent and summed in bfloat16 or wider, within the bound.
A program may use at most 128 MiB of HBM per device.

```python
import math
import jax
import jax.numpy as jnp
import numpy as np
from jax import lax

D = 2048
HEADS = 8
HEAD_DIM = 128
HG_WIDTH = 1024
BLOCK = 128
FFE = 512
FFS = 512
EXPERTS = 8
TOPK = 2
TOK_DEV = 512
ROWS = 128
TOKENS = 4096
SLICES = 4
CAP = 64
N_SP = 8
N_TP = 4


def forget_draw(key):
    noise_key, shift_key = jax.random.split(key)
    noise = jnp.clip(jax.random.normal(noise_key, (TOKENS, HG_WIDTH), jnp.float32), -6.0, 6.0)
    shifts = jax.random.uniform(shift_key, (TOKENS // TOK_DEV, 1, 1), jnp.float32, -1.5, 1.5)
    shaped = noise.reshape(TOKENS // TOK_DEV, TOK_DEV, HG_WIDTH) + shifts
    return shaped.reshape(TOKENS, HG_WIDTH).astype(jnp.bfloat16)


def draw_forget_ahead(key, part):
    return forget_draw(jax.random.fold_in(key, 101))


def draw_forget_behind(key, part):
    return forget_draw(jax.random.fold_in(key, 202))


def lower_bounds(key):
    pick_key, slow_key, fast_key, jitter_key = jax.random.split(key, 4)
    share = 0.5
    slow_heads = jax.random.uniform(pick_key, (HEADS, 1), jnp.float32) < share
    slow_gap = jnp.exp(jax.random.uniform(slow_key, (HEADS, 1), jnp.float32, jnp.log(0.2), jnp.log(1.0))) / TOKENS
    fast_gap = jnp.exp(jax.random.uniform(fast_key, (HEADS, 1), jnp.float32, jnp.log(0.02), jnp.log(0.08)))
    jitter = jnp.exp(jax.random.uniform(jitter_key, (HEADS, HEAD_DIM), jnp.float32, jnp.log(0.8), jnp.log(1.2)))
    gap_size = jnp.where(slow_heads, slow_gap, fast_gap) * jitter
    return (1.0 - gap_size).reshape(HG_WIDTH).astype(jnp.float32)


def draw_floor_ahead(key, part):
    return lower_bounds(jax.random.fold_in(key, 303))


def draw_floor_behind(key, part):
    return lower_bounds(jax.random.fold_in(key, 404))


def draw_decay_jolts(key, part):
    place_key, size_key = jax.random.split(jax.random.fold_in(key, 505))
    spots = jax.random.randint(place_key, (HEADS, 3), 0, TOKENS)
    losses = jnp.log(jax.random.uniform(size_key, (HEADS, 3), jnp.float32, 0.5, 0.8))
    head_rows = jnp.broadcast_to(jnp.arange(HEADS)[:, None], (HEADS, 3))
    return jnp.zeros((HEADS, TOKENS), jnp.float32).at[head_rows, spots].add(losses)


def steps_of(rng, shape, cuts, least, high):
    loudness, own = 1.0, jax.random.fold_in(rng, 6)
    for position, shards_of in cuts:
        heights = jnp.exp(jax.random.uniform(jax.random.fold_in(own, position), (shards_of,), jnp.float32, least / len(cuts), high / len(cuts)))
        loudness = loudness * jnp.repeat(heights, shape[position] // shards_of).reshape([-1 if axis == position else 1 for axis in range(len(shape))])
    return loudness


def shared_out(stream_key, own, number, rows, amount, top, bound, skew):
    sequence = jax.random.permutation(stream_key, amount)
    packed, common = shares(amount, rows * top, bound, skew, True), shares(amount, rows * top, bound, skew, False)
    places = jnp.arange(amount)

    def named(sizes, offset_by):
        used = int((sizes > 0).sum())
        fixed = max(1, used // 4)
        passed = fixed + (places - fixed + offset_by * (used - fixed)) % max(1, amount - fixed)
        return jnp.zeros((amount,), jnp.int32).at[sequence[jnp.where(places < fixed, places, passed)]].set(jnp.asarray(sizes, jnp.int32))

    sizes = jnp.where(number % 4 == 0, named(packed, number // 4), named(common, number - number // 4 - 1))
    mixed = jax.random.permutation(jax.random.fold_in(own, 3), amount)
    donor, sink = mixed[0:amount // 2 * 2:2], mixed[1:amount // 2 * 2:2]
    margin = jnp.minimum(sizes[donor] - 1, bound - sizes[sink]) // 2
    margin = jnp.where((donor == sequence[0]) | (sink == sequence[0]) | (sizes[sink] == 0), 0, jnp.maximum(margin, 0))
    passed = jax.random.randint(jax.random.fold_in(own, 4), (amount // 2,), 0, 1 << 20) % (margin + 1)
    sizes = sizes.at[donor].add(-passed).at[sink].add(passed)
    members = jnp.searchsorted(jnp.cumsum(sizes), jnp.arange(rows * top), side="right").astype(jnp.int32)
    listing = members.reshape(top, rows).T
    listing = listing[jax.random.permutation(jax.random.fold_in(own, 1), rows)]
    offset_by = jax.random.randint(jax.random.fold_in(own, 2), (rows, 1), 0, top)
    return jnp.take_along_axis(listing, (jnp.arange(top)[None, :] + offset_by) % top, axis=1)


def shares(amount, total, reach, slope, full):
    weights = [(1 << 20) // math.isqrt(rank ** slope) + 1 for rank in range(1, amount + 1)]
    largest = reach if full else min(reach, max(-(-total // amount), total * weights[0] // sum(weights)))
    least = 1 if total - largest >= amount - 1 else 0
    holding, rest = [largest] + [least] * (amount - 1), total - largest - least * (amount - 1)
    while rest > 0:
        candidates = [i for i in range(1, amount) if holding[i] < largest] or [i for i in range(1, amount) if holding[i] < reach]
        mass, remaining = sum([weights[i] for i in candidates]), rest
        for i in candidates:
            addition = min(reach - holding[i], max(1, remaining * weights[i] // mass), rest)
            holding[i] = holding[i] + addition
            rest = rest - addition
    return np.array(holding)


def normal_values(key, extent, deviation, bound, shards=(), kind=jnp.bfloat16):
    level = steps_of(key, extent, shards, -0.22, 0.18) if shards else 1.0
    values = jax.random.normal(key, extent, jnp.float32) * deviation * level
    return jnp.minimum(jnp.maximum(values, -bound), bound).astype(kind)


def setup_inputs(seed: int = 0) -> dict:
    key_list = jax.random.split(jax.random.key(seed), 22)
    query_input = normal_values(key_list[0], (TOKENS, HG_WIDTH), 1.0, 6.0, ((0, 8), (1, 4)))
    value_input = normal_values(key_list[1], (TOKENS, HG_WIDTH), 1.0, 6.0, ((0, 8), (1, 4)))
    forget_ahead = draw_forget_ahead(jax.random.fold_in(key_list[21], 71), 0)
    forget_behind = draw_forget_behind(jax.random.fold_in(key_list[21], 71), 0)
    output_gate = normal_values(key_list[4], (TOKENS, HG_WIDTH), 1.0, 6.0, ((0, 8), (1, 4)))
    floor_ahead = draw_floor_ahead(jax.random.fold_in(key_list[21], 71), 0)
    floor_behind = draw_floor_behind(jax.random.fold_in(key_list[21], 71), 0)
    head_gain = jnp.clip(1.0 + 0.18 * jax.random.normal(key_list[7], (HG_WIDTH,), jnp.float32), 0.1, 1.9)
    decay_jolts = draw_decay_jolts(jax.random.fold_in(key_list[21], 71), 0)
    residual = normal_values(key_list[9], (TOKENS, D), 1.0, 6.0, ((0, 32),))
    out_weight = normal_values(key_list[10], (HG_WIDTH, D), HG_WIDTH ** -0.5, 0.1875)
    norm_gain = jnp.clip(1.0 + 0.18 * jax.random.normal(key_list[11], (D,), jnp.float32), 0.1, 1.9)
    norm_bias = normal_values(key_list[12], (D,), 0.3, 1.5, (), jnp.float32)
    expert_ids_keys = jax.random.split(jax.random.fold_in(key_list[13], 1), TOKENS // ROWS)
    expert_ids_turns = jax.random.permutation(jax.random.fold_in(key_list[13], 3), TOKENS // ROWS)
    expert_ids = jax.vmap(lambda own, number: shared_out(jax.random.fold_in(key_list[13], 2), own, number, ROWS, EXPERTS, TOPK, CAP, 1))(expert_ids_keys, expert_ids_turns).reshape((TOKENS, TOPK))
    route_scale = jnp.clip(0.3 + 1.2 * jax.random.uniform(key_list[14], (TOKENS, TOPK), jnp.float32) ** steps_of(key_list[14], (TOKENS, TOPK), ((0, 8),), -0.2, 0.2), 0.3, 1.5)
    expert_gate = normal_values(key_list[15], (EXPERTS, D, FFE), D ** -0.5, 0.125, ((0, 8), (2, 4)))
    expert_up = normal_values(key_list[16], (EXPERTS, D, FFE), D ** -0.5, 0.125, ((0, 8), (2, 4)))
    expert_down = normal_values(key_list[17], (EXPERTS, FFE, D), FFE ** -0.5, 0.25, ((0, 8), (1, 4)))
    shared_gate = normal_values(key_list[18], (D, FFS), D ** -0.5, 0.125, ((1, 4),))
    shared_up = normal_values(key_list[19], (D, FFS), D ** -0.5, 0.125, ((1, 4),))
    shared_down = normal_values(key_list[20], (FFS, D), FFS ** -0.5, 0.25, ((0, 4),))
    return {"query_input": query_input, "value_input": value_input, "forget_ahead": forget_ahead, "forget_behind": forget_behind, "output_gate": output_gate, "floor_ahead": floor_ahead, "floor_behind": floor_behind, "head_gain": head_gain, "decay_jolts": decay_jolts, "residual": residual, "out_weight": out_weight, "norm_gain": norm_gain, "norm_bias": norm_bias, "expert_ids": expert_ids, "route_scale": route_scale, "expert_gate": expert_gate, "expert_up": expert_up, "expert_down": expert_down, "shared_gate": shared_gate, "shared_up": shared_up, "shared_down": shared_down}


epsilon = 1e-05
residual_scale = 2.0 ** 0.25
highest = lax.Precision.HIGHEST

def heads_first(source, head_count):
    length = source.shape[0]
    return source.astype(jnp.float32).reshape(length, head_count, -1).transpose(1, 0, 2)

def forget_terms(pre_gate, lower_bound, jolt_logs):
    forget_rate = (1.0 - lower_bound) * jax.nn.sigmoid(-pre_gate)
    return (forget_rate, jnp.log1p(-forget_rate) + jolt_logs)

def direction_terms(queries, keys_in, values, log_decay, block_len):
    head_count, length, state_width = queries.shape
    block_count = length // block_len

    def to_blocks(array):
        return array.reshape(head_count, block_count, block_len, array.shape[-1]).transpose(1, 0, 2, 3)
    query_blocks = to_blocks(queries)
    key_blocks = to_blocks(keys_in)
    value_blocks = to_blocks(values)
    cumulative = jnp.cumsum(to_blocks(log_decay), axis=2)
    middle = cumulative[:, :, block_len // 2 - 1:block_len // 2]
    block_end = cumulative[:, :, -1:]
    prefix = jnp.tril(jnp.ones((block_len, block_len), jnp.float32))
    scores = jnp.einsum('nhce,nhse->nhcs', query_blocks * jnp.exp(cumulative - middle), key_blocks * jnp.exp(middle - cumulative), precision=highest)
    within = jnp.einsum('nhcs,nhsv->nhcv', scores * prefix, value_blocks, precision=highest)
    query_start = query_blocks * jnp.exp(cumulative)
    key_end = key_blocks * jnp.exp(block_end - cumulative)
    decays = jnp.exp(block_end[:, :, 0])

    def advance(carry_state, pieces):
        query_piece, key_piece, value_piece, decay_piece = pieces
        readout = jnp.einsum('hce,hev->hcv', query_piece, carry_state, precision=highest)
        carry_state = decay_piece[..., None] * carry_state + jnp.einsum('hce,hcv->hev', key_piece, value_piece, precision=highest)
        return (carry_state, readout)
    zero_state = jnp.zeros((head_count, state_width, values.shape[-1]), jnp.float32)
    end_state, carried = lax.scan(advance, zero_state, (query_start, key_end, value_blocks, decays))
    block_out = (within + carried).transpose(1, 0, 2, 3).reshape(head_count, length, -1)
    decay_total = jnp.exp(lax.optimization_barrier(jnp.sum(log_decay, axis=1)))
    return (block_out, decay_total, end_state)

def finish_heads(summed, head_gain, gate_pre):
    head_count, length, state_width = summed.shape
    normed = summed * lax.rsqrt(lax.optimization_barrier(jnp.mean(summed * summed, axis=2, keepdims=True)) + epsilon)
    normed = normed * head_gain.reshape(head_count, 1, state_width)
    merged = normed.transpose(1, 0, 2).reshape(length, head_count * state_width)
    return (merged * jax.nn.silu(gate_pre.astype(jnp.float32))).astype(jnp.bfloat16)

def layer_norm(summed, norm_gain, norm_bias):
    centre = lax.optimization_barrier(jnp.mean(summed, axis=1, keepdims=True))
    shifted = summed - centre
    spread = lax.optimization_barrier(jnp.mean(shifted * shifted, axis=1, keepdims=True))
    return (shifted * lax.rsqrt(spread + epsilon) * norm_gain + norm_bias).astype(jnp.bfloat16)

def swiglu_sum(rows_in, gate_matrix, up_matrix, down_matrix, slice_count):
    gate_act = jnp.dot(rows_in, gate_matrix, preferred_element_type=jnp.float32)
    upward = jnp.dot(rows_in, up_matrix, preferred_element_type=jnp.float32)
    hidden = (jax.nn.silu(gate_act) * upward).astype(jnp.bfloat16)
    piece_width = hidden.shape[1] // slice_count
    running = jnp.zeros((rows_in.shape[0], down_matrix.shape[1]), jnp.float32)
    for part_index in range(slice_count):
        partial_term = jnp.dot(hidden[:, part_index * piece_width:(part_index + 1) * piece_width], down_matrix[part_index * piece_width:(part_index + 1) * piece_width], preferred_element_type=jnp.float32)
        running = running + lax.optimization_barrier(partial_term.astype(jnp.bfloat16)).astype(jnp.float32)
    return running

def slot_ranks(chosen, expert_count):
    flat_ids = chosen.reshape(-1)
    one_hot = (flat_ids[:, None] == jnp.arange(expert_count, dtype=jnp.int32)[None, :]).astype(jnp.int32)
    before = jnp.cumsum(one_hot, axis=0) - one_hot
    return lax.optimization_barrier(jnp.sum(before * one_hot, axis=1)).astype(jnp.int32)

def slot_sources(targets, top_count, slot_total):
    owners = jnp.arange(targets.shape[0], dtype=jnp.int32) // top_count
    source = jnp.zeros((slot_total,), jnp.int32).at[targets].set(owners)
    filled = jnp.zeros((slot_total,), jnp.int32).at[targets].set(1)
    return (source, filled)

def reference(query_input, value_input, forget_ahead, forget_behind, output_gate, floor_ahead, floor_behind, head_gain, decay_jolts, residual, out_weight, norm_gain, norm_bias, expert_ids, route_scale, expert_gate, expert_up, expert_down, shared_gate, shared_up, shared_down):
    head_count = decay_jolts.shape[0]
    queries = jax.nn.silu(heads_first(query_input, head_count))
    values = heads_first(value_input, head_count)
    state_width = queries.shape[2]
    jolt_logs = decay_jolts[:, :, None]
    rate_ahead, log_ahead = forget_terms(heads_first(forget_ahead, head_count), floor_ahead.reshape(head_count, 1, state_width), jolt_logs)
    rate_behind, log_behind = forget_terms(jnp.flip(heads_first(forget_behind, head_count), 1), floor_behind.reshape(head_count, 1, state_width), jnp.flip(jolt_logs, 1))
    ahead_out = direction_terms(queries, rate_ahead, values, log_ahead, BLOCK)[0]
    behind_out = direction_terms(jnp.flip(queries, 1), rate_behind, jnp.flip(values, 1), log_behind, BLOCK)[0]
    mixed_rows = finish_heads(ahead_out + jnp.flip(behind_out, 1), head_gain, output_gate)
    projected = jnp.dot(mixed_rows, out_weight, preferred_element_type=jnp.float32)
    normed_rows = layer_norm(residual_scale * residual.astype(jnp.float32) + projected, norm_gain, norm_bias)
    blocks = N_SP * N_TP
    block_ids = expert_ids.reshape(blocks, ROWS, TOPK)
    slot_rank = jax.vmap(lambda chosen: slot_ranks(chosen, EXPERTS))(block_ids)
    lane_size = blocks * CAP
    targets = (block_ids.reshape(blocks, ROWS * TOPK) * lane_size + jnp.arange(blocks, dtype=jnp.int32)[:, None] * CAP + slot_rank).reshape(-1).astype(jnp.int32)
    source, filled = slot_sources(targets, TOPK, EXPERTS * lane_size)

    def run_expert(pieces):
        gate_matrix, up_matrix, down_matrix, source_rows, filled_rows = pieces
        taken_rows = jnp.take(normed_rows, source_rows, axis=0)
        rows_in = jnp.where(filled_rows[:, None] > 0, taken_rows, jnp.zeros_like(taken_rows))
        return swiglu_sum(rows_in, gate_matrix, up_matrix, down_matrix, SLICES).astype(jnp.bfloat16)
    expert_out = lax.map(run_expert, (expert_gate, expert_up, expert_down, source.reshape(EXPERTS, lane_size), filled.reshape(EXPERTS, lane_size)))
    picked = jnp.take(expert_out.reshape(EXPERTS * lane_size, D), targets, axis=0)
    picked = picked.astype(jnp.float32).reshape(TOKENS, TOPK, D)
    routed = lax.optimization_barrier(jnp.sum(picked * route_scale[:, :, None], axis=1))
    shared = swiglu_sum(normed_rows, shared_gate, shared_up, shared_down, SLICES)
    return (residual_scale * normed_rows.astype(jnp.float32) + shared + routed).astype(jnp.bfloat16)
```

```python
import jax
import jax.numpy as jnp
from jax import lax
from jax.sharding import PartitionSpec as P

BLOCK = 128


epsilon = 1e-05
residual_scale = 2.0**0.25
highest = lax.Precision.HIGHEST


def shifted_in(value, axis, distance, reverse):
    count = lax.axis_size(axis)
    if reverse:
        pairs = [(i + distance, i) for i in range(count - distance)]
    else:
        pairs = [(i, i + distance) for i in range(count - distance)]
    decay, state = value
    packed = jnp.concatenate([state, decay[:, :, None]], axis=2).astype(jnp.bfloat16)
    moved = lax.ppermute(packed, axis, pairs).astype(jnp.float32)
    width = state.shape[2]
    return (moved[:, :, width], moved[:, :, :width])


def carried_in(both, axis):
    count = lax.axis_size(axis)
    both = [shifted_in(value, axis, 1, bool(k)) for k, value in enumerate(both)]
    distance = 1
    while distance < count - 1:
        both = [
            chain_states(shifted_in(value, axis, distance, bool(k)), value)
            for k, value in enumerate(both)
        ]
        distance *= 2
    return both


def heads_first(source, head_count):
    length = source.shape[0]
    return source.astype(jnp.float32).reshape(length, head_count, -1).transpose(1, 0, 2)


def forget_terms(pre_gate, lower_bound, jolt_logs):
    forget_rate = (1.0 - lower_bound) * jax.nn.sigmoid(-pre_gate)
    return (forget_rate, jnp.log1p(-forget_rate) + jolt_logs)


def direction_terms(queries, keys_in, values, log_decay, block_len):
    head_count, length, state_width = queries.shape
    block_count = length // block_len

    def to_blocks(array):
        return array.reshape(head_count, block_count, block_len, array.shape[-1]).transpose(
            1, 0, 2, 3
        )

    query_blocks = to_blocks(queries)
    key_blocks = to_blocks(keys_in)
    value_blocks = to_blocks(values)
    cumulative = jnp.cumsum(to_blocks(log_decay), axis=2)
    middle = cumulative[:, :, block_len // 2 - 1 : block_len // 2]
    block_end = cumulative[:, :, -1:]
    prefix = jnp.tril(jnp.ones((block_len, block_len), jnp.float32))
    scores = jnp.einsum(
        "nhce,nhse->nhcs",
        query_blocks * jnp.exp(cumulative - middle),
        key_blocks * jnp.exp(middle - cumulative),
        precision=highest,
    )
    within = jnp.einsum("nhcs,nhsv->nhcv", scores * prefix, value_blocks, precision=highest)
    query_start = query_blocks * jnp.exp(cumulative)
    key_end = key_blocks * jnp.exp(block_end - cumulative)
    decays = jnp.exp(block_end[:, :, 0])

    def advance(carry_state, pieces):
        query_piece, key_piece, value_piece, decay_piece = pieces
        readout = jnp.einsum("hce,hev->hcv", query_piece, carry_state, precision=highest)
        carry_state = decay_piece[..., None] * carry_state + jnp.einsum(
            "hce,hcv->hev", key_piece, value_piece, precision=highest
        )
        return (carry_state, readout)

    zero_state = jnp.zeros((head_count, state_width, values.shape[-1]), jnp.float32)
    end_state, carried = lax.scan(advance, zero_state, (query_start, key_end, value_blocks, decays))
    block_out = (within + carried).transpose(1, 0, 2, 3).reshape(head_count, length, -1)
    decay_total = jnp.exp(jnp.sum(log_decay, axis=1))
    return (block_out, decay_total, end_state)


def chain_states(earlier, following):
    return (earlier[0] * following[0], following[0][..., None] * earlier[1] + following[1])


def carried_readout(queries, log_decay, entering):
    return jnp.einsum(
        "hle,hev->hlv",
        queries * jnp.exp(jnp.cumsum(log_decay, axis=1)),
        entering,
        precision=highest,
    )


def finish_heads(summed, head_gain, gate_pre):
    head_count, length, state_width = summed.shape
    normed = summed * lax.rsqrt(jnp.mean(summed * summed, axis=2, keepdims=True) + epsilon)
    normed = normed * head_gain.reshape(head_count, 1, state_width)
    merged = normed.transpose(1, 0, 2).reshape(length, head_count * state_width)
    return (merged * jax.nn.silu(gate_pre.astype(jnp.float32))).astype(jnp.bfloat16)


def layer_norm(summed, norm_gain, norm_bias):
    centre = jnp.mean(summed, axis=1, keepdims=True)
    shifted = summed - centre
    spread = jnp.mean(shifted * shifted, axis=1, keepdims=True)
    return (shifted * lax.rsqrt(spread + epsilon) * norm_gain + norm_bias).astype(jnp.bfloat16)


def slot_ranks(chosen, expert_count):
    flat_ids = chosen.reshape(-1)
    one_hot = (flat_ids[:, None] == jnp.arange(expert_count, dtype=jnp.int32)[None, :]).astype(
        jnp.int32
    )
    before = jnp.cumsum(one_hot, axis=0) - one_hot
    return jnp.sum(before * one_hot, axis=1)


def fill_slots(rows_in, targets, top_count, slot_total):
    owners = jnp.arange(targets.shape[0], dtype=jnp.int32) // top_count
    source = jnp.zeros((slot_total,), jnp.int32).at[targets].set(owners)
    filled = jnp.zeros((slot_total,), jnp.int32).at[targets].set(1)
    taken_rows = jnp.take(rows_in, source, axis=0)
    return jnp.where(filled[:, None] > 0, taken_rows, jnp.zeros_like(taken_rows))


def shared_whole(shared_input, shared_gate, shared_up, shared_down):
    shared_act = jnp.dot(shared_input, shared_gate, preferred_element_type=jnp.float32)
    shared_upward = jnp.dot(shared_input, shared_up, preferred_element_type=jnp.float32)
    shared_hidden = (jax.nn.silu(shared_act) * shared_upward).astype(jnp.bfloat16)
    return jnp.dot(shared_hidden, shared_down, preferred_element_type=jnp.float32)


def local(
    query_input,
    value_input,
    forget_ahead,
    forget_behind,
    output_gate,
    floor_ahead,
    floor_behind,
    head_gain,
    decay_jolts,
    residual,
    out_weight,
    norm_gain,
    norm_bias,
    expert_ids,
    route_scale,
    expert_gate,
    expert_up,
    expert_down,
    shared_gate,
    shared_up,
    shared_down,
):
    wide_gate = lax.all_gather(expert_gate, "tp", axis=2, tiled=True)
    wide_up = lax.all_gather(expert_up, "tp", axis=2, tiled=True)
    wide_shared_gate = lax.all_gather(shared_gate, "tp", axis=1, tiled=True)
    wide_shared_up = lax.all_gather(shared_up, "tp", axis=1, tiled=True)
    wide_down = lax.all_gather(expert_down, "tp", axis=1, tiled=True)
    wide_shared_down = lax.all_gather(shared_down, "tp", axis=0, tiled=True)
    head_count = decay_jolts.shape[0]
    queries = jax.nn.silu(heads_first(query_input, head_count))
    values = heads_first(value_input, head_count)
    state_width = queries.shape[2]
    jolt_logs = decay_jolts[:, :, None]
    rate_ahead, log_ahead = forget_terms(
        heads_first(forget_ahead, head_count),
        floor_ahead.reshape(head_count, 1, state_width),
        jolt_logs,
    )
    rate_behind, log_behind = forget_terms(
        jnp.flip(heads_first(forget_behind, head_count), 1),
        floor_behind.reshape(head_count, 1, state_width),
        jnp.flip(jolt_logs, 1),
    )
    mirrored = jnp.flip(queries, 1)
    ahead_out, ahead_decay, ahead_state = direction_terms(
        queries, rate_ahead, values, log_ahead, BLOCK
    )
    behind_out, behind_decay, behind_state = direction_terms(
        mirrored, rate_behind, jnp.flip(values, 1), log_behind, BLOCK
    )
    entering_ahead, entering_behind = carried_in(
        ((ahead_decay, ahead_state), (behind_decay, behind_state)), "sp"
    )
    ahead_out = ahead_out + carried_readout(queries, log_ahead, entering_ahead[1])
    behind_out = behind_out + carried_readout(mirrored, log_behind, entering_behind[1])
    mixed_rows = finish_heads(ahead_out + jnp.flip(behind_out, 1), head_gain, output_gate)
    local_rows = residual.shape[0]
    model_width = residual.shape[1]
    own_mixed = lax.all_to_all(mixed_rows, "tp", split_axis=0, concat_axis=1, tiled=True)
    projected = jnp.dot(own_mixed, out_weight, preferred_element_type=jnp.float32)
    normed_rows = layer_norm(
        residual_scale * residual.astype(jnp.float32) + projected, norm_gain, norm_bias
    )
    sp_count = lax.axis_size("sp")
    tp_count = lax.axis_size("tp")
    tp_index = lax.axis_index("tp")
    local_experts = expert_gate.shape[0]
    expert_count = local_experts * sp_count
    top_count = expert_ids.shape[1]
    capacity = 2 * local_rows * top_count // expert_count
    block_ids = expert_ids.reshape(tp_count, local_rows, top_count)
    own_ids = lax.dynamic_index_in_dim(block_ids, tp_index, 0, keepdims=False)
    own_scale = lax.dynamic_index_in_dim(
        route_scale.reshape(tp_count, local_rows, top_count), tp_index, 0, keepdims=False
    )
    own_ranks = slot_ranks(own_ids, expert_count)
    own_targets = own_ids.reshape(-1) * capacity + own_ranks
    outgoing = fill_slots(normed_rows, own_targets, top_count, expert_count * capacity)
    arrived = lax.all_to_all(outgoing, "sp", split_axis=0, concat_axis=0, tiled=True)
    grouped = arrived.reshape(sp_count, local_experts, capacity, model_width)
    gate_act = jnp.einsum("semd,edf->semf", grouped, wide_gate, preferred_element_type=jnp.float32)
    upward = jnp.einsum("semd,edf->semf", grouped, wide_up, preferred_element_type=jnp.float32)
    hidden = (jax.nn.silu(gate_act) * upward).astype(jnp.bfloat16)
    routed_sum = jnp.einsum(
        "semf,efd->semd", hidden, wide_down, preferred_element_type=jnp.float32
    )
    came_back = lax.all_to_all(
        routed_sum.astype(jnp.bfloat16).reshape(-1, model_width),
        "sp",
        split_axis=0,
        concat_axis=0,
        tiled=True,
    )
    shared_sum = shared_whole(normed_rows, wide_shared_gate, wide_shared_up, wide_shared_down)
    picked = jnp.take(came_back, own_targets, axis=0).astype(jnp.float32)
    picked = picked.reshape(local_rows, top_count, model_width)
    routed = jnp.sum(picked * own_scale[:, :, None], axis=1)
    return (residual_scale * normed_rows.astype(jnp.float32) + shared_sum + routed).astype(
        jnp.bfloat16
    )


def solution(mesh):
    in_specs = (
        P("sp", "tp"),
        P("sp", "tp"),
        P("sp", "tp"),
        P("sp", "tp"),
        P("sp", "tp"),
        P("tp"),
        P("tp"),
        P("tp"),
        P("tp", "sp"),
        P(("sp", "tp"), None),
        P(),
        P(),
        P(),
        P("sp", None),
        P("sp", None),
        P("sp", None, "tp"),
        P("sp", None, "tp"),
        P("sp", "tp", None),
        P(None, "tp"),
        P(None, "tp"),
        P("tp", None),
    )
    out_specs = P(("sp", "tp"), None)
    return jax.shard_map(local, mesh=mesh, in_specs=in_specs, out_specs=out_specs, check_vma=False)
```

```python
import jax
import jax.numpy as jnp
from jax import lax
from jax.sharding import PartitionSpec as P

BLOCK = 128


epsilon = 1e-05
residual_scale = 2.0**0.25
highest = lax.Precision.HIGHEST


def shifted_in(value, axis, distance, reverse):
    count = lax.axis_size(axis)
    if reverse:
        pairs = [(i + distance, i) for i in range(count - distance)]
    else:
        pairs = [(i, i + distance) for i in range(count - distance)]
    decay, state = value
    packed = jnp.concatenate([state, decay[:, :, None]], axis=2).astype(jnp.bfloat16)
    moved = lax.ppermute(packed, axis, pairs).astype(jnp.float32)
    width = state.shape[2]
    return (moved[:, :, width], moved[:, :, :width])


def carried_in(both, axis):
    count = lax.axis_size(axis)
    both = [shifted_in(value, axis, 1, bool(k)) for k, value in enumerate(both)]
    distance = 1
    while distance < count - 1:
        both = [
            chain_states(shifted_in(value, axis, distance, bool(k)), value)
            for k, value in enumerate(both)
        ]
        distance *= 2
    return both


def heads_first(source, head_count):
    length = source.shape[0]
    return source.astype(jnp.float32).reshape(length, head_count, -1).transpose(1, 0, 2)


def forget_terms(pre_gate, lower_bound, jolt_logs):
    forget_rate = (1.0 - lower_bound) * jax.nn.sigmoid(-pre_gate)
    return (forget_rate, jnp.log1p(-forget_rate) + jolt_logs)


def direction_terms(queries, keys_in, values, log_decay, block_len):
    head_count, length, state_width = queries.shape
    block_count = length // block_len

    def to_blocks(array):
        return array.reshape(head_count, block_count, block_len, array.shape[-1]).transpose(
            1, 0, 2, 3
        )

    query_blocks = to_blocks(queries)
    key_blocks = to_blocks(keys_in)
    value_blocks = to_blocks(values)
    cumulative = jnp.cumsum(to_blocks(log_decay), axis=2)
    middle = cumulative[:, :, block_len // 2 - 1 : block_len // 2]
    block_end = cumulative[:, :, -1:]
    prefix = jnp.tril(jnp.ones((block_len, block_len), jnp.float32))
    scores = jnp.einsum(
        "nhce,nhse->nhcs",
        query_blocks * jnp.exp(cumulative - middle),
        key_blocks * jnp.exp(middle - cumulative),
        precision=highest,
    )
    within = jnp.einsum("nhcs,nhsv->nhcv", scores * prefix, value_blocks, precision=highest)
    query_start = query_blocks * jnp.exp(cumulative)
    key_end = key_blocks * jnp.exp(block_end - cumulative)
    decays = jnp.exp(block_end[:, :, 0])
    added = jnp.einsum("nhce,nhcv->nhev", key_end, value_blocks, precision=highest)
    end_state = added[0]
    decay_total = decays[0]
    for n in range(1, block_count):
        decay_total, end_state = chain_states((decay_total, end_state), (decays[n], added[n]))
    return (within, query_start, decays, added, (decay_total, end_state))


def chain_states(earlier, following):
    return (earlier[0] * following[0], following[0][..., None] * earlier[1] + following[1])


def with_entering(within, query_start, decays, added, entering):
    states = [entering]
    for n in range(decays.shape[0] - 1):
        states.append(decays[n][..., None] * states[-1] + added[n])
    carried = jnp.einsum("nhce,nhev->nhcv", query_start, jnp.stack(states), precision=highest)
    block_count, head_count, block_len, width = within.shape
    return (within + carried).transpose(1, 0, 2, 3).reshape(
        head_count, block_count * block_len, width
    )


def finish_heads(summed, head_gain, gate_pre):
    head_count, length, state_width = summed.shape
    normed = summed * lax.rsqrt(jnp.mean(summed * summed, axis=2, keepdims=True) + epsilon)
    normed = normed * head_gain.reshape(head_count, 1, state_width)
    merged = normed.transpose(1, 0, 2).reshape(length, head_count * state_width)
    return (merged * jax.nn.silu(gate_pre.astype(jnp.float32))).astype(jnp.bfloat16)


def layer_norm(summed, norm_gain, norm_bias):
    centre = jnp.mean(summed, axis=1, keepdims=True)
    shifted = summed - centre
    spread = jnp.mean(shifted * shifted, axis=1, keepdims=True)
    return (shifted * lax.rsqrt(spread + epsilon) * norm_gain + norm_bias).astype(jnp.bfloat16)


def slot_ranks(chosen, expert_count):
    flat_ids = chosen.reshape(-1)
    one_hot = (flat_ids[:, None] == jnp.arange(expert_count, dtype=jnp.int32)[None, :]).astype(
        jnp.int32
    )
    before = jnp.cumsum(one_hot, axis=0) - one_hot
    return jnp.sum(before * one_hot, axis=1)


def fill_slots(rows_in, targets, top_count, slot_total):
    owners = jnp.arange(targets.shape[0], dtype=jnp.int32) // top_count
    source = jnp.zeros((slot_total,), jnp.int32).at[targets].set(owners)
    filled = jnp.zeros((slot_total,), jnp.int32).at[targets].set(1)
    taken_rows = jnp.take(rows_in, source, axis=0)
    return jnp.where(filled[:, None] > 0, taken_rows, jnp.zeros_like(taken_rows))


def shared_whole(shared_input, shared_gate, shared_up, shared_down):
    shared_act = jnp.dot(shared_input, shared_gate, preferred_element_type=jnp.float32)
    shared_upward = jnp.dot(shared_input, shared_up, preferred_element_type=jnp.float32)
    shared_hidden = (jax.nn.silu(shared_act) * shared_upward).astype(jnp.bfloat16)
    return jnp.dot(shared_hidden, shared_down, preferred_element_type=jnp.float32)


def local(
    query_input,
    value_input,
    forget_ahead,
    forget_behind,
    output_gate,
    floor_ahead,
    floor_behind,
    head_gain,
    decay_jolts,
    residual,
    out_weight,
    norm_gain,
    norm_bias,
    expert_ids,
    route_scale,
    expert_gate,
    expert_up,
    expert_down,
    shared_gate,
    shared_up,
    shared_down,
):
    wide_gate = lax.all_gather(expert_gate, "tp", axis=2, tiled=True)
    wide_up = lax.all_gather(expert_up, "tp", axis=2, tiled=True)
    wide_shared_gate = lax.all_gather(shared_gate, "tp", axis=1, tiled=True)
    wide_shared_up = lax.all_gather(shared_up, "tp", axis=1, tiled=True)
    wide_down = lax.all_gather(expert_down, "tp", axis=1, tiled=True)
    wide_shared_down = lax.all_gather(shared_down, "tp", axis=0, tiled=True)
    head_count = decay_jolts.shape[0]
    queries = jax.nn.silu(heads_first(query_input, head_count))
    values = heads_first(value_input, head_count)
    state_width = queries.shape[2]
    jolt_logs = decay_jolts[:, :, None]
    rate_ahead, log_ahead = forget_terms(
        heads_first(forget_ahead, head_count),
        floor_ahead.reshape(head_count, 1, state_width),
        jolt_logs,
    )
    rate_behind, log_behind = forget_terms(
        jnp.flip(heads_first(forget_behind, head_count), 1),
        floor_behind.reshape(head_count, 1, state_width),
        jnp.flip(jolt_logs, 1),
    )
    within, query_start, decays, added, (total, ends) = direction_terms(
        jnp.concatenate([queries, jnp.flip(queries, 1)]),
        jnp.concatenate([rate_ahead, rate_behind]),
        jnp.concatenate([values, jnp.flip(values, 1)]),
        jnp.concatenate([log_ahead, log_behind]),
        BLOCK,
    )
    entering = carried_in(
        ((total[:head_count], ends[:head_count]), (total[head_count:], ends[head_count:])), "sp"
    )
    outs = with_entering(
        within, query_start, decays, added, jnp.concatenate([entering[0][1], entering[1][1]])
    )
    ahead_out, behind_out = (outs[:head_count], outs[head_count:])
    mixed_rows = finish_heads(ahead_out + jnp.flip(behind_out, 1), head_gain, output_gate)
    local_rows = residual.shape[0]
    model_width = residual.shape[1]
    own_mixed = lax.all_to_all(mixed_rows, "tp", split_axis=0, concat_axis=1, tiled=True)
    projected = jnp.dot(own_mixed, out_weight, preferred_element_type=jnp.float32)
    normed_rows = layer_norm(
        residual_scale * residual.astype(jnp.float32) + projected, norm_gain, norm_bias
    )
    sp_count = lax.axis_size("sp")
    tp_count = lax.axis_size("tp")
    tp_index = lax.axis_index("tp")
    local_experts = expert_gate.shape[0]
    expert_count = local_experts * sp_count
    top_count = expert_ids.shape[1]
    capacity = 2 * local_rows * top_count // expert_count
    block_ids = expert_ids.reshape(tp_count, local_rows, top_count)
    own_ids = lax.dynamic_index_in_dim(block_ids, tp_index, 0, keepdims=False)
    own_scale = lax.dynamic_index_in_dim(
        route_scale.reshape(tp_count, local_rows, top_count), tp_index, 0, keepdims=False
    )
    own_ranks = slot_ranks(own_ids, expert_count)
    own_targets = own_ids.reshape(-1) * capacity + own_ranks
    outgoing = fill_slots(normed_rows, own_targets, top_count, expert_count * capacity)
    arrived = lax.all_to_all(outgoing, "sp", split_axis=0, concat_axis=0, tiled=True)
    grouped = arrived.reshape(sp_count, local_experts, capacity, model_width)
    gate_act = jnp.einsum("semd,edf->semf", grouped, wide_gate, preferred_element_type=jnp.float32)
    upward = jnp.einsum("semd,edf->semf", grouped, wide_up, preferred_element_type=jnp.float32)
    hidden = (jax.nn.silu(gate_act) * upward).astype(jnp.bfloat16)
    routed_sum = jnp.einsum(
        "semf,efd->semd", hidden, wide_down, preferred_element_type=jnp.float32
    )
    came_back = lax.all_to_all(
        routed_sum.astype(jnp.bfloat16).reshape(-1, model_width),
        "sp",
        split_axis=0,
        concat_axis=0,
        tiled=True,
    )
    shared_sum = shared_whole(normed_rows, wide_shared_gate, wide_shared_up, wide_shared_down)
    picked = jnp.take(came_back, own_targets, axis=0).astype(jnp.float32)
    picked = picked.reshape(local_rows, top_count, model_width)
    routed = jnp.sum(picked * own_scale[:, :, None], axis=1)
    return (residual_scale * normed_rows.astype(jnp.float32) + shared_sum + routed).astype(
        jnp.bfloat16
    )


def solution(mesh):
    in_specs = (
        P("sp", "tp"),
        P("sp", "tp"),
        P("sp", "tp"),
        P("sp", "tp"),
        P("sp", "tp"),
        P("tp"),
        P("tp"),
        P("tp"),
        P("tp", "sp"),
        P(("sp", "tp"), None),
        P(),
        P(),
        P(),
        P("sp", None),
        P("sp", None),
        P("sp", None, "tp"),
        P("sp", None, "tp"),
        P("sp", "tp", None),
        P(None, "tp"),
        P(None, "tp"),
        P("tp", None),
    )
    out_specs = P(("sp", "tp"), None)
    return jax.shard_map(local, mesh=mesh, in_specs=in_specs, out_specs=out_specs, check_vma=False)
```
